32 devices in a mesh: sp: 8 (over z, x), tp: 4 (over y, core).
Axes of the slice: x: 2, y: 2, z: 4, core: 2. Of those that a mesh axis runs over, the one named last changes fastest.
Arguments:
- tokens: bfloat16 [2048, 1024], P(('sp', 'tp')), may hold values from -6 to 6
- norm_gain: float32 [1024], replicated, may hold values from 0.1 to 1.9
- w_query: bfloat16 [1024, 1024], P('sp', 'tp'), may hold values from -0.1875 to 0.1875
- w_key: bfloat16 [1024, 1024], P('sp', 'tp'), may hold values from -0.1875 to 0.1875
- w_value: bfloat16 [1024, 1024], P('sp', 'tp'), may hold values from -0.1875 to 0.1875
- w_forget: bfloat16 [1024, 16], P('sp', 'tp'), may hold values from -0.375 to 0.375
- forget_offset: float32 [16], P('tp'), may hold values from 1 to 3.5
- w_out_t: bfloat16 [1024, 1024], P('sp', 'tp'), may hold values from -0.1875 to 0.1875
- out_gain: float32 [1024], replicated, may hold values from 0.1 to 1.9
Outputs:
- mixed: bfloat16 [2048, 1024], P(('sp', 'tp'))
The draws below stay inside these ranges and needn't reach their ends.
All inputs are finite; a program needn't handle non-finite values.
Results may differ from the reference program's by a relative error of at most 0.015.
Values may be sent and summed in bfloat16 or wider, within the bound.
A program may use at most 192 MiB of HBM per device.

```python
import jax
import jax.numpy as jnp
from jax import lax

D = 1024
HEADS = 16
HEAD_DIM = 64
TOK_DEV = 256
TOKENS = 2048
N_SP = 8


def block_scale(key, dims, split, smallest, top_value):
    def one(axis_at, blocks):
        draws = jax.random.uniform(jax.random.fold_in(jax.random.fold_in(key, 6), axis_at), (blocks,), jnp.float32, smallest / len(split), top_value / len(split))
        return jnp.repeat(jnp.exp(draws), dims[axis_at] // blocks).reshape((-1,) + (1,) * (len(dims) - axis_at - 1))

    loudness = one(*split[0])
    for cut in split[1:]:
        loudness = loudness * one(*cut)
    return loudness


def gaussian(rng, shape, spread, limit, shards=(), kind=jnp.bfloat16):
    drawn = jax.random.normal(rng, shape, jnp.float32) * spread
    if len(shards) > 0:
        drawn = block_scale(rng, shape, shards, -0.22, 0.18) * drawn
    return jnp.clip(drawn, min=-limit, max=limit).astype(kind)


def setup_inputs(seed: int = 0) -> dict:
    streams_of = jax.random.split(jax.random.key(seed), 10)
    tokens = gaussian(streams_of[0], (TOKENS, D), 1.0, 6.0, ((0, 32),))
    norm_gain = jnp.clip(1.0 + 0.18 * jax.random.normal(streams_of[1], (D,), jnp.float32), 0.1, 1.9)
    w_query = gaussian(streams_of[2], (D, HEADS * HEAD_DIM), D ** -0.5, 0.1875, ((0, 8), (1, 4)))
    w_key = gaussian(streams_of[3], (D, HEADS * HEAD_DIM), D ** -0.5, 0.1875, ((0, 8), (1, 4)))
    w_value = gaussian(streams_of[4], (D, HEADS * HEAD_DIM), D ** -0.5, 0.1875, ((0, 8), (1, 4)))
    w_forget = gaussian(streams_of[5], (D, HEADS), (D // 4) ** -0.5, 0.375, ((0, 8), (1, 4)))
    forget_offset = jnp.clip(1.0 + 2.5 * jax.random.uniform(streams_of[6], (HEADS,), jnp.float32) ** block_scale(streams_of[6], (HEADS,), ((0, 4),), -0.2, 0.2), 1.0, 3.5)
    w_out_t = gaussian(streams_of[7], (D, HEADS * HEAD_DIM), (HEADS * HEAD_DIM) ** -0.5, 0.1875, ((0, 8), (1, 4)))
    out_gain = jnp.clip(1.0 + 0.18 * jax.random.normal(streams_of[8], (D,), jnp.float32), 0.1, 1.9)
    return {"tokens": tokens, "norm_gain": norm_gain, "w_query": w_query, "w_key": w_key, "w_value": w_value, "w_forget": w_forget, "forget_offset": forget_offset, "w_out_t": w_out_t, "out_gain": out_gain}


norm_eps = 1e-06

def rms_norm(values_in, gain_row):
    floats = values_in.astype(jnp.float32)
    scale_row = lax.rsqrt(lax.optimization_barrier(jnp.mean(floats * floats, axis=-1, keepdims=True)) + norm_eps)
    return (floats * scale_row * gain_row).astype(jnp.bfloat16)

def reference(tokens, norm_gain, w_query, w_key, w_value, w_forget, forget_offset, w_out_t, out_gain):
    normed = rms_norm(tokens, norm_gain)
    queries = jnp.dot(normed, w_query, preferred_element_type=jnp.float32).astype(jnp.bfloat16)
    keys_all = jnp.dot(normed, w_key, preferred_element_type=jnp.float32).astype(jnp.bfloat16)
    values_all = jnp.dot(normed, w_value, preferred_element_type=jnp.float32).astype(jnp.bfloat16)
    logits = jnp.dot(normed, w_forget, preferred_element_type=jnp.float32) + forget_offset + jnp.log(jnp.float32(TOKENS))
    log_gates = jax.nn.log_sigmoid(logits)
    cumulative = jnp.cumsum(log_gates, axis=0)
    head_shape = (TOKENS, HEADS, HEAD_DIM)
    key_heads = keys_all.reshape(head_shape).astype(jnp.float32)
    value_heads = values_all.reshape(head_shape).astype(jnp.float32)
    query_blocks = queries.reshape(N_SP, TOK_DEV, HEADS, HEAD_DIM).astype(jnp.float32)
    cum_blocks = cumulative.reshape(N_SP, TOK_DEV, HEADS)
    key_pos = jnp.arange(TOKENS, dtype=jnp.int32)

    def attend(block_args):
        query_block, cum_block, block_index = block_args
        scores = jnp.einsum('qhd,khd->hqk', query_block, key_heads, precision=lax.Precision.HIGHEST) * HEAD_DIM ** (-0.5)
        scores = scores + cum_block.T[:, :, None] - cumulative.T[:, None, :]
        query_pos = block_index * TOK_DEV + jnp.arange(TOK_DEV, dtype=jnp.int32)
        allowed = key_pos[None, :] <= query_pos[:, None]
        scores = jnp.where(allowed[None], scores, -jnp.inf)
        attn_probs = jax.nn.softmax(scores, axis=-1)
        return jnp.einsum('hqk,khd->qhd', attn_probs, value_heads, precision=lax.Precision.HIGHEST)
    attended = lax.map(attend, (query_blocks, cum_blocks, jnp.arange(N_SP, dtype=jnp.int32)))
    attended = attended.reshape(TOKENS, HEADS * HEAD_DIM).astype(jnp.bfloat16)
    projected = lax.dot_general(attended, w_out_t, (((1,), (1,)), ((), ())), preferred_element_type=jnp.float32)
    return rms_norm(projected, out_gain)
```

```python
import functools

import jax
import jax.numpy as jnp
from jax import lax
from jax.experimental import pallas as pl
from jax.experimental.pallas import tpu as pltpu
from jax.sharding import PartitionSpec as P

HEAD_DIM = 64
LANES = 128
NORM_EPS = 1e-06
MESH = pl.DeviceIdType.MESH
F32 = jnp.float32
BF16 = jnp.bfloat16
CONTRACT_LAST = (((1,), (1,)), ((), ()))


def rms_norm(floats, gain_row):
    scale_col = lax.rsqrt(jnp.mean(floats * floats, axis=-1, keepdims=True) + NORM_EPS)
    return (floats * scale_col * gain_row).astype(BF16)


def layer_kernel(
    n_sp, n_tp, heads,
    tokens_ref, gain_ref, wq_ref, wk_ref, wv_ref, wf_ref, offset_ref, wo_ref, out_gain_ref,
    out_ref,
    normed, w_all, wo_all, kv_all, gates, q_heads, cum_query, run_max, run_acc, partial, shares,
    local_sem, send_sem, recv_sem, gate_send, gate_recv, tok_send, tok_recv, sum_send, sum_recv,
):
    sp, tp = lax.axis_index("sp"), lax.axis_index("tp")
    rows = tokens_ref.shape[0]
    w_rows, width = wq_ref.shape
    block = rows * n_tp
    half = n_sp // 2

    odd = lax.rem(sp, 2)
    place = (1 - odd) * lax.div(sp, 2) + odd * (n_sp - lax.div(sp + 1, 2))

    def index_at(position):
        position = lax.rem(position + n_sp, n_sp)
        upper = lax.div(position, half)
        return (1 - upper) * 2 * position + upper * (2 * (n_sp - position) - 1)

    right, left = index_at(place + 1), index_at(place - 1)

    def shard_w(index):
        return w_all.at[pl.ds(pl.multiple_of(index * w_rows, w_rows), w_rows), :]

    def shard_wo(index):
        return wo_all.at[pl.ds(pl.multiple_of(index * w_rows, w_rows), w_rows), :]

    def shard_kv(index):
        return kv_all.at[pl.ds(pl.multiple_of(index * block, block), block), :]

    def hop(ring, shard, way, step, index):
        return pltpu.make_async_remote_copy(
            src_ref=shard(index),
            dst_ref=shard(index),
            send_sem=send_sem.at[ring, way, step],
            recv_sem=recv_sem.at[ring, way, step],
            device_id=((right, left)[way], tp),
            device_id_type=MESH,
        )

    def ring_start(ring, shard):
        hop(ring, shard, 0, 1, sp).start()
        if half > 1:
            hop(ring, shard, 1, 1, sp).start()

    def ring_step(ring, shard, step):
        first, second = index_at(place - step), index_at(place + step)
        hop(ring, shard, 0, step, first).wait_recv()

        @pl.when(step < half)
        def _():
            hop(ring, shard, 0, step + 1, first).start()
            hop(ring, shard, 1, step, second).wait_recv()

        @pl.when(step < half - 1)
        def _():
            hop(ring, shard, 1, step + 1, second).start()

        return first, second

    def ring_drain(ring, shard):
        @pl.loop(1, half + 1)
        def _(step):
            hop(ring, shard, 0, step, sp).wait_send()

            @pl.when(step < half)
            def _():
                hop(ring, shard, 1, step, sp).wait_send()

    own_rows = pl.ds(pl.multiple_of(sp * w_rows, w_rows), w_rows)
    local = [
        pltpu.make_async_copy(ref, w_all.at[own_rows, pl.ds(i * width, width)], local_sem.at[i])
        for i, ref in enumerate((wq_ref, wk_ref, wv_ref))
    ]
    local.append(pltpu.make_async_copy(wo_ref, wo_all.at[own_rows, :], local_sem.at[3]))
    for copy in local:
        copy.start()

    barrier = pltpu.get_barrier_semaphore()
    for shift in range(1, n_sp):
        pl.semaphore_signal(
            barrier, inc=1, device_id=(lax.rem(sp + shift, n_sp), tp), device_id_type=MESH
        )
    for shift in range(1, n_tp):
        pl.semaphore_signal(
            barrier, inc=1, device_id=(sp, lax.rem(tp + shift, n_tp)), device_id_type=MESH
        )

    forget = jnp.concatenate(
        [wf_ref[...].astype(F32), jnp.zeros((w_rows, LANES - heads), F32)], axis=1
    )
    w_all[own_rows, 3 * width :] = forget.astype(BF16)
    my_rows = pl.ds(pl.multiple_of(tp * rows, rows), rows)
    normed[my_rows, :] = rms_norm(tokens_ref[...].astype(F32), gain_ref[...])
    for copy in local:
        copy.wait()
    pl.semaphore_wait(barrier, n_sp + n_tp - 2)

    ring_start(0, shard_w)

    def tok_copy(shift):
        return pltpu.make_async_remote_copy(
            src_ref=normed.at[my_rows, :],
            dst_ref=normed.at[my_rows, :],
            send_sem=tok_send.at[shift - 1],
            recv_sem=tok_recv.at[shift - 1],
            device_id=(sp, lax.rem(tp + shift, n_tp)),
            device_id_type=MESH,
        )

    for shift in range(1, n_tp):
        tok_copy(shift).start()

    @pl.loop(1, half + 1)
    def _(step):
        ring_step(0, shard_w, step)

    for shift in range(1, n_tp):
        tok_copy(shift).wait()

    tokens_here = normed[...]
    own_block = pl.ds(pl.multiple_of(sp * block, block), block)
    kv_all[own_block, :] = jnp.dot(
        tokens_here, w_all[:, width : 3 * width], preferred_element_type=F32
    ).astype(BF16)
    logits = jnp.dot(tokens_here, w_all[:, 3 * width :], preferred_element_type=F32)
    lane_row = lax.broadcasted_iota(jnp.int32, (1, LANES), 1)
    offset_row = jnp.zeros((1, LANES), F32)
    for h in range(heads):
        offset_row = jnp.where(lane_row == h, offset_ref[h], offset_row)
    logits = logits + offset_row + jnp.log(jnp.full((1, LANES), n_sp * block, F32))
    log_gates = jnp.minimum(logits, 0.0) - jnp.log1p(jnp.exp(-jnp.abs(logits)))
    row_at = lax.broadcasted_iota(jnp.int32, (block, block), 0)
    col_at = lax.broadcasted_iota(jnp.int32, (block, block), 1)
    seen = col_at <= row_at
    ring_start(1, shard_kv)
    cum_here = jnp.dot(
        jnp.where(seen, 1.0, 0.0).astype(F32), log_gates,
        precision=lax.Precision.HIGHEST, preferred_element_type=F32,
    )
    cum_query[...] = cum_here
    gates[pl.ds(sp, 1)] = cum_here.T[None, :8, :]
    queries = (
        jnp.dot(tokens_here, w_all[:, :width], preferred_element_type=F32).astype(BF16).astype(F32)
        * HEAD_DIM ** (-0.5)
    )
    head_at = lax.broadcasted_iota(jnp.int32, (block, width), 1) // HEAD_DIM
    for h in range(heads):
        q_heads[h] = jnp.where(head_at == h, queries, 0.0).astype(BF16)

    def gate_copy(shift):
        return pltpu.make_async_remote_copy(
            src_ref=gates.at[pl.ds(sp, 1)],
            dst_ref=gates.at[pl.ds(sp, 1)],
            send_sem=gate_send.at[shift - 1],
            recv_sem=gate_recv.at[shift - 1],
            device_id=(lax.rem(sp + shift, n_sp), tp),
            device_id_type=MESH,
        )

    for shift in range(1, n_sp):
        gate_copy(shift).start()
    ring_start(2, shard_wo)

    def scores_of(h, index):
        key_block = kv_all[pl.ds(pl.multiple_of(index * block, block), block), :width]
        scores = lax.dot_general(
            q_heads[h], key_block, CONTRACT_LAST, preferred_element_type=F32
        )
        return scores + cum_query[:, h : h + 1] - gates[index, h : h + 1, :]

    def weighted(h, index, weights):
        value_block = kv_all[pl.ds(pl.multiple_of(index * block, block), block), width:]
        with_ones = jnp.where(head_at == h, value_block.astype(F32), 1.0).astype(BF16)
        return jnp.dot(weights.astype(BF16), with_ones, preferred_element_type=F32)

    for h in range(heads):
        scores = jnp.where(seen, scores_of(h, sp), -1e30)
        top = jnp.max(scores, axis=-1, keepdims=True)
        run_max[h] = top
        run_acc[h] = weighted(h, sp, jnp.where(seen, jnp.exp(scores - top), 0.0))

    def absorb(index):
        for h in range(heads):
            scores = scores_of(h, index)
            old = run_max[h]
            top = jnp.maximum(old, jnp.max(scores, axis=-1, keepdims=True))
            run_max[h] = top
            run_acc[h] = run_acc[h] * jnp.exp(old - top) + weighted(
                h, index, jnp.exp(scores - top)
            )

    for shift in range(1, n_sp):
        gate_copy(shift).wait()

    def shift_back(count, start):
        index = sp - 1 - count
        local_cum = gates[index]
        start = start - local_cum[:, block - 1 :]
        gates[index] = local_cum + start
        return start

    lax.fori_loop(0, sp, shift_back, jnp.zeros((8, 1), F32))

    @pl.loop(1, half + 1)
    def _(step):
        first, second = ring_step(1, shard_kv, step)

        @pl.when(first < sp)
        def _():
            absorb(first)

        @pl.when((step < half) & (second < sp))
        def _():
            absorb(second)

        ring_step(2, shard_wo, step)

    attended = jnp.zeros((block, width), F32)
    for h in range(heads):
        other = ((h + 1) % heads) * HEAD_DIM
        acc = run_acc[h]
        attended = jnp.where(head_at == h, acc / acc[:, other : other + 1], attended)
    partial[...] = lax.dot_general(
        attended.astype(BF16), wo_all[...], CONTRACT_LAST, preferred_element_type=F32
    ).astype(BF16)

    def sum_copy(shift):
        peer = lax.rem(tp + shift, n_tp)
        return pltpu.make_async_remote_copy(
            src_ref=partial.at[pl.ds(pl.multiple_of(peer * rows, rows), rows), :],
            dst_ref=shares.at[shift - 1],
            send_sem=sum_send.at[shift - 1],
            recv_sem=sum_recv.at[shift - 1],
            device_id=(sp, peer),
            device_id_type=MESH,
        )

    for shift in range(1, n_tp):
        sum_copy(shift).start()
    ring_drain(0, shard_w)
    ring_drain(1, shard_kv)
    ring_drain(2, shard_wo)
    total = partial[my_rows, :].astype(F32)
    for shift in range(1, n_tp):
        sum_copy(shift).wait()
        total = total + shares[shift - 1].astype(F32)
    out_ref[...] = rms_norm(total, out_gain_ref[...])


def solution(mesh):
    n_sp, n_tp = mesh.shape["sp"], mesh.shape["tp"]

    def on_device(
        tokens, norm_gain, w_query, w_key, w_value, w_forget, forget_offset, w_out_t, out_gain
    ):
        rows, model = tokens.shape
        w_rows, width = w_query.shape
        heads = w_forget.shape[1]
        block = rows * n_tp
        steps = n_sp // 2 + 1
        vmem = pl.BlockSpec(memory_space=pltpu.VMEM)
        anywhere = pl.BlockSpec(memory_space=pl.ANY)
        dma = pltpu.SemaphoreType.DMA
        return pl.pallas_call(
            functools.partial(layer_kernel, n_sp, n_tp, heads),
            out_shape=jax.ShapeDtypeStruct((rows, model), BF16),
            in_specs=[
                vmem, vmem, anywhere, anywhere, anywhere, vmem,
                pl.BlockSpec(memory_space=pltpu.SMEM), anywhere, vmem,
            ],
            out_specs=vmem,
            scratch_shapes=[
                pltpu.VMEM((block, model), BF16),
                pltpu.VMEM((n_sp * w_rows, 3 * width + LANES), BF16),
                pltpu.VMEM((n_sp * w_rows, width), BF16),
                pltpu.VMEM((n_sp * block, 2 * width), BF16),
                pltpu.VMEM((n_sp, 8, block), F32),
                pltpu.VMEM((heads, block, width), BF16),
                pltpu.VMEM((block, LANES), F32),
                pltpu.VMEM((heads, block, 1), F32),
                pltpu.VMEM((heads, block, width), F32),
                pltpu.VMEM((block, model), BF16),
                pltpu.VMEM((n_tp - 1, rows, model), BF16),
                dma((4,)),
                dma((3, 2, steps)),
                dma((3, 2, steps)),
                dma((n_sp - 1,)),
                dma((n_sp - 1,)),
                dma((n_tp - 1,)),
                dma((n_tp - 1,)),
                dma((n_tp - 1,)),
                dma((n_tp - 1,)),
            ],
            compiler_params=pltpu.CompilerParams(collective_id=0, has_side_effects=True),
        )(
            tokens, norm_gain.reshape(1, model), w_query, w_key, w_value, w_forget,
            forget_offset, w_out_t, out_gain.reshape(1, model),
        )

    return jax.shard_map(
        on_device,
        mesh=mesh,
        in_specs=(
            P(("sp", "tp"), None),
            P(),
            P("sp", "tp"),
            P("sp", "tp"),
            P("sp", "tp"),
            P("sp", "tp"),
            P("tp"),
            P("sp", "tp"),
            P(),
        ),
        out_specs=P(("sp", "tp"), None),
        check_vma=False,
    )
```

```python
import functools

import jax
import jax.numpy as jnp
from jax import lax
from jax.experimental import pallas as pl
from jax.experimental.pallas import tpu as pltpu
from jax.sharding import PartitionSpec as P

HEAD_DIM = 64
LANES = 128
NORM_EPS = 1e-06
MESH = pl.DeviceIdType.MESH
F32 = jnp.float32
BF16 = jnp.bfloat16
CONTRACT_LAST = (((1,), (1,)), ((), ()))


def rms_norm(floats, gain_row):
    scale_col = lax.rsqrt(jnp.mean(floats * floats, axis=-1, keepdims=True) + NORM_EPS)
    return (floats * scale_col * gain_row).astype(BF16)


def layer_kernel(
    n_sp, n_tp, heads,
    tokens_ref, gain_ref, wq_ref, wk_ref, wv_ref, wf_ref, offset_ref, wo_ref, out_gain_ref,
    out_ref,
    normed, w_all, wo_all, kv_all, forget_all, gates, q_heads, cum_query, run_max, run_acc, partial, shares,
    local_sem, send_sem, recv_sem, forget_send, forget_recv, gate_send, gate_recv, tok_send, tok_recv, sum_send, sum_recv,
):
    sp, tp = lax.axis_index("sp"), lax.axis_index("tp")
    rows = tokens_ref.shape[0]
    w_rows, width = wq_ref.shape
    block = rows * n_tp
    half = n_sp // 2

    odd = lax.rem(sp, 2)
    place = (1 - odd) * lax.div(sp, 2) + odd * (n_sp - lax.div(sp + 1, 2))

    def index_at(position):
        position = lax.rem(position + n_sp, n_sp)
        upper = lax.div(position, half)
        return (1 - upper) * 2 * position + upper * (2 * (n_sp - position) - 1)

    right, left = index_at(place + 1), index_at(place - 1)

    def view(ref, index, count, chunk):
        lanes = ref.shape[1] // 2
        return ref.at[
            pl.ds(pl.multiple_of(index * count, count), count), pl.ds(chunk * lanes, lanes)
        ]

    def hop(ring, chunk, way, step, index):
        ref, count = ((w_all, w_rows), (kv_all, block), (wo_all, w_rows))[ring]
        return pltpu.make_async_remote_copy(
            src_ref=view(ref, index, count, chunk),
            dst_ref=view(ref, index, count, chunk),
            send_sem=send_sem.at[ring, chunk, way, step],
            recv_sem=recv_sem.at[ring, chunk, way, step],
            device_id=((right, left)[way], tp),
            device_id_type=MESH,
        )

    lanes_of_ring = [(c, w, half if c == w else half - 1) for c in (0, 1) for w in (c, 1 - c)]

    def ring_start(ring):
        for chunk, way, last in lanes_of_ring:
            if last > 0:
                hop(ring, chunk, way, 1, sp).start()

    def ring_step(ring, step):
        arrived = index_at(place - step), index_at(place + step)
        for chunk, way, last in lanes_of_ring:

            @pl.when(step <= last)
            def _():
                hop(ring, chunk, way, step, arrived[way]).wait_recv()

                @pl.when(step < last)
                def _():
                    hop(ring, chunk, way, step + 1, arrived[way]).start()

        return arrived

    def ring_drain(ring):
        for chunk, way, last in lanes_of_ring:

            @pl.loop(1, last + 1)
            def _(step):
                hop(ring, chunk, way, step, sp).wait_send()

    own_rows = pl.ds(pl.multiple_of(sp * w_rows, w_rows), w_rows)
    local = [
        pltpu.make_async_copy(ref, w_all.at[own_rows, pl.ds(i * width, width)], local_sem.at[i])
        for i, ref in enumerate((wq_ref, wk_ref, wv_ref))
    ]
    local.append(pltpu.make_async_copy(wo_ref, wo_all.at[own_rows, :], local_sem.at[3]))
    for copy in local:
        copy.start()

    barrier = pltpu.get_barrier_semaphore()
    for shift in range(1, n_sp):
        pl.semaphore_signal(
            barrier, inc=1, device_id=(lax.rem(sp + shift, n_sp), tp), device_id_type=MESH
        )
    for shift in range(1, n_tp):
        pl.semaphore_signal(
            barrier, inc=1, device_id=(sp, lax.rem(tp + shift, n_tp)), device_id_type=MESH
        )

    forget_all[pl.ds(sp, 1)] = jnp.concatenate(
        [wf_ref[...].astype(F32), jnp.zeros((8 - heads, w_rows), F32)], axis=0
    )[None]
    my_rows = pl.ds(pl.multiple_of(tp * rows, rows), rows)
    normed[my_rows, :] = rms_norm(tokens_ref[...].astype(F32), gain_ref[...])
    for copy in local:
        copy.wait()
    pl.semaphore_wait(barrier, n_sp + n_tp - 2)

    def spread(ref, sends, receives):
        return [
            pltpu.make_async_remote_copy(
                src_ref=ref.at[pl.ds(sp, 1)],
                dst_ref=ref.at[pl.ds(sp, 1)],
                send_sem=sends.at[shift - 1],
                recv_sem=receives.at[shift - 1],
                device_id=(lax.rem(sp + shift, n_sp), tp),
                device_id_type=MESH,
            )
            for shift in range(1, n_sp)
        ]

    forget_copies = spread(forget_all, forget_send, forget_recv)
    for copy in forget_copies:
        copy.start()

    def tok_copy(shift):
        return pltpu.make_async_remote_copy(
            src_ref=normed.at[my_rows, :],
            dst_ref=normed.at[my_rows, :],
            send_sem=tok_send.at[shift - 1],
            recv_sem=tok_recv.at[shift - 1],
            device_id=(sp, lax.rem(tp + shift, n_tp)),
            device_id_type=MESH,
        )

    for shift in range(1, n_tp):
        tok_copy(shift).start()
    ring_start(0)

    @pl.loop(1, half)
    def _(step):
        ring_step(0, step)

    for shift in range(1, n_tp):
        tok_copy(shift).wait()
    for copy in forget_copies:
        copy.wait()

    tokens_here = normed[...]
    forget_rows = jnp.concatenate([forget_all[i] for i in range(n_sp)], axis=1).astype(BF16)
    logits = lax.dot_general(
        forget_rows, tokens_here, CONTRACT_LAST, preferred_element_type=F32
    )
    head_row = lax.broadcasted_iota(jnp.int32, (8, block), 0)
    offsets = jnp.zeros((8, block), F32)
    for h in range(heads):
        offsets = jnp.where(head_row == h, offset_ref[h], offsets)
    logits = logits + offsets + jnp.log(jnp.full((8, block), n_sp * block, F32))
    log_gates = jnp.minimum(logits, 0.0) - jnp.log1p(jnp.exp(-jnp.abs(logits)))
    row_at = lax.broadcasted_iota(jnp.int32, (block, block), 0)
    col_at = lax.broadcasted_iota(jnp.int32, (block, block), 1)
    seen = col_at <= row_at
    cum_here = jnp.dot(
        log_gates, jnp.where(row_at <= col_at, 1.0, 0.0).astype(F32),
        precision=lax.Precision.HIGHEST, preferred_element_type=F32,
    )
    gates[pl.ds(sp, 1)] = cum_here[None]
    cum_query[...] = jnp.concatenate([cum_here, jnp.zeros((LANES - 8, block), F32)], axis=0).T
    gate_copies = spread(gates, gate_send, gate_recv)
    for copy in gate_copies:
        copy.start()
    ring_step(0, half)

    ring_start(2)
    own_block = pl.ds(pl.multiple_of(sp * block, block), block)
    kv_all[own_block, :] = jnp.dot(
        tokens_here, w_all[:, width:], preferred_element_type=F32
    ).astype(BF16)
    ring_start(1)
    queries = (
        jnp.dot(tokens_here, w_all[:, :width], preferred_element_type=F32).astype(BF16).astype(F32)
        * HEAD_DIM ** (-0.5)
    )
    head_at = lax.broadcasted_iota(jnp.int32, (block, width), 1) // HEAD_DIM
    for h in range(heads):
        q_heads[h] = jnp.where(head_at == h, queries, 0.0).astype(BF16)

    def scores_of(h, index):
        key_block = kv_all[pl.ds(pl.multiple_of(index * block, block), block), :width]
        scores = lax.dot_general(
            q_heads[h], key_block, CONTRACT_LAST, preferred_element_type=F32
        )
        return scores + cum_query[:, h : h + 1] - gates[index, h : h + 1, :]

    def weighted(h, index, weights):
        value_block = kv_all[pl.ds(pl.multiple_of(index * block, block), block), width:]
        with_ones = jnp.where(head_at == h, value_block.astype(F32), 1.0).astype(BF16)
        return jnp.dot(weights.astype(BF16), with_ones, preferred_element_type=F32)

    for h in range(heads):
        scores = jnp.where(seen, scores_of(h, sp), -1e30)
        top = jnp.max(scores, axis=-1, keepdims=True)
        run_max[h] = top
        run_acc[h] = weighted(h, sp, jnp.where(seen, jnp.exp(scores - top), 0.0))

    def absorb(index):
        for h in range(heads):
            scores = scores_of(h, index)
            old = run_max[h]
            top = jnp.maximum(old, jnp.max(scores, axis=-1, keepdims=True))
            run_max[h] = top
            run_acc[h] = run_acc[h] * jnp.exp(old - top) + weighted(
                h, index, jnp.exp(scores - top)
            )

    for copy in gate_copies:
        copy.wait()

    def shift_back(count, start):
        index = sp - 1 - count
        local_cum = gates[index]
        start = start - local_cum[:, block - 1 :]
        gates[index] = local_cum + start
        return start

    lax.fori_loop(0, sp, shift_back, jnp.zeros((8, 1), F32))
    ring_step(2, 1)

    @pl.loop(1, half + 1)
    def _(step):
        first, second = ring_step(1, step)

        @pl.when(first < sp)
        def _():
            absorb(first)

        @pl.when((step < half) & (second < sp))
        def _():
            absorb(second)

        @pl.when(step < half)
        def _():
            ring_step(2, step + 1)

    attended = jnp.zeros((block, width), F32)
    for h in range(heads):
        other = ((h + 1) % heads) * HEAD_DIM
        acc = run_acc[h]
        attended = jnp.where(head_at == h, acc / acc[:, other : other + 1], attended)
    partial[...] = lax.dot_general(
        attended.astype(BF16), wo_all[...], CONTRACT_LAST, preferred_element_type=F32
    ).astype(BF16)

    def sum_copy(shift):
        peer = lax.rem(tp + shift, n_tp)
        return pltpu.make_async_remote_copy(
            src_ref=partial.at[pl.ds(pl.multiple_of(peer * rows, rows), rows), :],
            dst_ref=shares.at[shift - 1],
            send_sem=sum_send.at[shift - 1],
            recv_sem=sum_recv.at[shift - 1],
            device_id=(sp, peer),
            device_id_type=MESH,
        )

    for shift in range(1, n_tp):
        sum_copy(shift).start()
    for ring in range(3):
        ring_drain(ring)
    total = partial[my_rows, :].astype(F32)
    for shift in range(1, n_tp):
        sum_copy(shift).wait()
        total = total + shares[shift - 1].astype(F32)
    out_ref[...] = rms_norm(total, out_gain_ref[...])


def solution(mesh):
    n_sp, n_tp = mesh.shape["sp"], mesh.shape["tp"]

    def on_device(
        tokens, norm_gain, w_query, w_key, w_value, w_forget, forget_offset, w_out_t, out_gain
    ):
        rows, model = tokens.shape
        w_rows, width = w_query.shape
        heads = w_forget.shape[1]
        block = rows * n_tp
        steps = n_sp // 2 + 1
        vmem = pl.BlockSpec(memory_space=pltpu.VMEM)
        anywhere = pl.BlockSpec(memory_space=pl.ANY)
        dma = pltpu.SemaphoreType.DMA
        return pl.pallas_call(
            functools.partial(layer_kernel, n_sp, n_tp, heads),
            out_shape=jax.ShapeDtypeStruct((rows, model), BF16),
            in_specs=[
                vmem, vmem, anywhere, anywhere, anywhere, vmem,
                pl.BlockSpec(memory_space=pltpu.SMEM), anywhere, vmem,
            ],
            out_specs=vmem,
            scratch_shapes=[
                pltpu.VMEM((block, model), BF16),
                pltpu.VMEM((n_sp * w_rows, 3 * width), BF16),
                pltpu.VMEM((n_sp * w_rows, width), BF16),
                pltpu.VMEM((n_sp * block, 2 * width), BF16),
                pltpu.VMEM((n_sp, 8, w_rows), F32),
                pltpu.VMEM((n_sp, 8, block), F32),
                pltpu.VMEM((heads, block, width), BF16),
                pltpu.VMEM((block, LANES), F32),
                pltpu.VMEM((heads, block, 1), F32),
                pltpu.VMEM((heads, block, width), F32),
                pltpu.VMEM((block, model), BF16),
                pltpu.VMEM((n_tp - 1, rows, model), BF16),
                dma((4,)),
                dma((3, 2, 2, steps)),
                dma((3, 2, 2, steps)),
                dma((n_sp - 1,)),
                dma((n_sp - 1,)),
                dma((n_sp - 1,)),
                dma((n_sp - 1,)),
                dma((n_tp - 1,)),
                dma((n_tp - 1,)),
                dma((n_tp - 1,)),
                dma((n_tp - 1,)),
            ],
            compiler_params=pltpu.CompilerParams(collective_id=0, has_side_effects=True),
        )(
            tokens, norm_gain.reshape(1, model), w_query, w_key, w_value, w_forget.T,
            forget_offset, w_out_t, out_gain.reshape(1, model),
        )

    return jax.shard_map(
        on_device,
        mesh=mesh,
        in_specs=(
            P(("sp", "tp"), None),
            P(),
            P("sp", "tp"),
            P("sp", "tp"),
            P("sp", "tp"),
            P("sp", "tp"),
            P("tp"),
            P("sp", "tp"),
            P(),
        ),
        out_specs=P(("sp", "tp"), None),
        check_vma=False,
    )
```
